32 devices in a mesh: grp: 2 (over y), sp: 4 (over z), tp: 4 (over x, core).
Axes of the slice: x: 2, y: 2, z: 4, core: 2. Of those that a mesh axis runs over, the one named last changes fastest.
Arguments:
- resid_in: bfloat16 [2048, 2048], P(('grp', 'sp', 'tp')), parts along dimension 0, may hold values from -6 to 6
- query_narrow: bfloat16 [2048, 8, 128], P(('grp', 'sp'), 'tp'), parts along dimension 0, may hold values from -512 to 512
- key_narrow: bfloat16 [2048, 4, 128], P(('grp', 'sp'), 'tp'), parts along dimension 0, may hold values from -512 to 512
- value_narrow: bfloat16 [2048, 4, 128], P(('grp', 'sp'), 'tp'), parts along dimension 0, may hold values from -6 to 6
- query_wide: bfloat16 [2048, 8, 256], P(('grp', 'sp'), 'tp'), parts along dimension 0, may hold values from -512 to 512
- key_wide: bfloat16 [2048, 4, 256], P(('grp', 'sp'), 'tp'), parts along dimension 0, may hold values from -512 to 512
- value_wide: bfloat16 [2048, 4, 128], P(('grp', 'sp'), 'tp'), parts along dimension 0, may hold values from -6 to 6
- lambda_narrow: float32 [8], P('tp'), may hold values from 0.3 to 0.8
- lambda_wide: float32 [8], P('tp'), may hold values from 0.3 to 0.8
- head_gain: float32 [128], replicated, may hold values from 0.1 to 1.9
- out_narrow: bfloat16 [1024, 2048], P('tp'), may hold values from -0.125 to 0.125
- out_wide: bfloat16 [1024, 2048], P('tp'), may hold values from -0.125 to 0.125
- norm_gain: bfloat16 [2048], replicated, may hold values from 0.099609375 to 1.8984375
- up_weight: bfloat16 [2048, 8192], P('sp', 'tp'), may hold values from -0.125 to 0.125
- down_weight: bfloat16 [8192, 2048], P('tp', 'sp'), may hold values from -0.0625 to 0.0625
Outputs:
- mixed_out: bfloat16 [2048, 2048], P(('grp', 'sp', 'tp')), parts along dimension 0
The draws below stay inside these ranges and needn't reach their ends.
There are 2 independent parts, one for each index of `grp`. The reference program is written for one: setup_inputs(seed, part) draws one part's arguments, and reference() takes and returns one part's arrays. A program takes and returns all parts, laid end to end along the dimension named above; an argument that names none is the same for every part. Nothing has to cross between parts.
All inputs are finite; a program needn't handle non-finite values.
Results may differ from the reference program's by a relative error of at most 0.018.
Values may be sent and summed in bfloat16 or wider, within the bound.
A program may use at most 128 MiB of HBM per device.

```python
import math
import jax
import jax.numpy as jnp
from jax import lax

D = 2048
FF = 8192
HN = 8
DN = 64
KN = 4
HW = 8
DW = 128
KW = 4
DV = 128
SEQ = 1024
N_TP = 4


SPREAD = 1.32


def paired_draw(base_key, head_count, key_head_stack, half_width):
    full_width = 2 * half_width
    query_draw, keys_draw = jax.random.split(base_key, 2)
    key_rows = jnp.clip(jax.random.normal(keys_draw, (SEQ, key_head_stack, full_width), jnp.float32) * SPREAD, -4.0 * SPREAD, 4.0 * SPREAD)
    query_rows_all = jnp.clip(jax.random.normal(query_draw, (SEQ, head_count, full_width), jnp.float32) * SPREAD, -4.0 * SPREAD, 4.0 * SPREAD)
    return (query_rows_all, key_rows)


def draw_query_narrow(key, part):
    return paired_draw(jax.random.fold_in(key, 101), HN, KN, DN)[0].astype(jnp.bfloat16)


def draw_key_narrow(key, part):
    return paired_draw(jax.random.fold_in(key, 101), HN, KN, DN)[1].astype(jnp.bfloat16)


def draw_query_wide(key, part):
    return paired_draw(jax.random.fold_in(key, 202), HW, KW, DW)[0].astype(jnp.bfloat16)


def draw_key_wide(key, part):
    return paired_draw(jax.random.fold_in(key, 202), HW, KW, DW)[1].astype(jnp.bfloat16)


def steps_of(rng, shape, cuts, smallest, high):
    level = 1.0
    for dim, shards_of in cuts:
        steps = jax.random.uniform(jax.random.fold_in(jax.random.fold_in(rng, 6), dim), (shards_of,), jnp.float32, smallest / len(cuts), high / len(cuts))
        level = level * jnp.repeat(jnp.exp(steps), shape[dim] // shards_of).reshape((-1,) + (1,) * (len(shape) - 1 - dim))
    return level


def scatter_about(key, dims, spread, limit, cuts=(), held_as=jnp.bfloat16):
    result = jax.random.normal(key, dims, jnp.float32) * spread
    if len(cuts) > 0:
        result = steps_of(key, dims, cuts, -0.22, 0.18) * result
    return jnp.clip(result, min=-limit, max=limit).astype(held_as)


def setup_inputs(seed: int = 0, part: int = 0) -> dict:
    streams_of = jax.random.split(jax.random.key(seed), 16)
    part_splits = jax.random.split(jax.random.fold_in(streams_of[15], part), 16)
    return {
        "resid_in": scatter_about(part_splits[0], (SEQ, D), 1.0, 6.0, ((0, 16),)),
        "query_narrow": draw_query_narrow(jax.random.fold_in(jax.random.fold_in(streams_of[15], part), 71), part),
        "key_narrow": draw_key_narrow(jax.random.fold_in(jax.random.fold_in(streams_of[15], part), 71), part),
        "value_narrow": scatter_about(part_splits[3], (SEQ, KN, DV), 1.0, 6.0, ((0, 4), (1, 4))),
        "query_wide": draw_query_wide(jax.random.fold_in(jax.random.fold_in(streams_of[15], part), 71), part),
        "key_wide": draw_key_wide(jax.random.fold_in(jax.random.fold_in(streams_of[15], part), 71), part),
        "value_wide": scatter_about(part_splits[6], (SEQ, KW, DV), 1.0, 6.0, ((0, 4), (1, 4))),
        "lambda_narrow": jnp.clip(0.3 + 0.5 * jax.random.uniform(streams_of[7], (HN,), jnp.float32) ** steps_of(streams_of[7], (HN,), ((0, 4),), -0.2, 0.2), 0.3, 0.8),
        "lambda_wide": jnp.clip(0.3 + 0.5 * jax.random.uniform(streams_of[8], (HW,), jnp.float32) ** steps_of(streams_of[8], (HW,), ((0, 4),), -0.2, 0.2), 0.3, 0.8),
        "head_gain": jnp.clip(1.0 + 0.18 * jax.random.normal(streams_of[9], (DV,), jnp.float32), 0.1, 1.9),
        "out_narrow": scatter_about(streams_of[10], (HN * DV, D), ((HN + HW) * DV) ** -0.5, 0.125, ((0, 4),)),
        "out_wide": scatter_about(streams_of[11], (HW * DV, D), ((HN + HW) * DV) ** -0.5, 0.125, ((0, 4),)),
        "norm_gain": jnp.clip(1.0 + 0.18 * jax.random.normal(streams_of[12], (D,), jnp.float32), 0.099609375, 1.8984375).astype(jnp.bfloat16),
        "up_weight": scatter_about(streams_of[13], (D, FF), D ** -0.5, 0.125, ((0, 4), (1, 4))),
        "down_weight": scatter_about(streams_of[14], (FF, D), FF ** -0.5, 0.0625, ((0, 4), (1, 4))),
    }


NORM_EPS = 1e-06
OUT_SCALE = 0.8

def attend_ref(query, key_rows, values, lambdas, gain_vec):
    seq_len, head_count, full_width = query.shape
    key_head_stack = key_rows.shape[1]
    half_width = full_width // 2
    group_size = head_count // key_head_stack
    value_width = values.shape[2]
    block_rows = math.gcd(seq_len, 128)
    rotation_count = seq_len // block_rows
    key_float32 = key_rows.astype(jnp.float32).reshape(seq_len, key_head_stack, 2, half_width)
    value_float32 = values.astype(jnp.float32)
    query_blocks = query.reshape(rotation_count, block_rows, key_head_stack, group_size, 2, half_width)
    lambda_grid = lambdas.reshape(key_head_stack, group_size)[:, :, None, None]

    def per_block(query_blk):
        scores = jnp.einsum('tkgcd,skcd->kgcts', query_blk.astype(jnp.float32), key_float32) * half_width ** (-0.5)
        row_top = lax.optimization_barrier(jnp.max(scores, axis=-1, keepdims=True))
        powers = jnp.exp(scores - row_top)
        row_total = lax.optimization_barrier(jnp.sum(powers, axis=-1))
        rounded_result = lax.optimization_barrier(powers.astype(jnp.bfloat16)).astype(jnp.float32)
        weighted_values = jnp.einsum('iodph,hie->iodpe', rounded_result, value_float32)
        first_map = weighted_values[:, :, 0] / row_total[:, :, 0, :, None]
        second_map = weighted_values[:, :, 1] / row_total[:, :, 1, :, None]
        mixed = first_map - lambda_grid * second_map
        normed = mixed * lax.rsqrt(lax.optimization_barrier(jnp.mean(mixed * mixed, axis=-1, keepdims=True)) + NORM_EPS) * gain_vec * OUT_SCALE
        normed = normed.astype(jnp.bfloat16).transpose(2, 0, 1, 3)
        return normed.reshape(block_rows, head_count, value_width)
    outcome = lax.map(per_block, query_blocks)
    return outcome.reshape(seq_len, head_count * value_width)

def rounded_add(running, partial_value):
    return running + lax.optimization_barrier(partial_value.astype(jnp.bfloat16)).astype(jnp.float32)

def reference(resid_in, query_narrow, key_narrow, value_narrow, query_wide, key_wide, value_wide, lambda_narrow, lambda_wide, head_gain, out_narrow, out_wide, norm_gain, up_weight, down_weight):
    att_narrow = attend_ref(query_narrow, key_narrow, value_narrow, lambda_narrow, head_gain)
    att_wide = attend_ref(query_wide, key_wide, value_wide, lambda_wide, head_gain)
    narrow_cols = att_narrow.shape[1] // N_TP
    wide_cols = att_wide.shape[1] // N_TP
    projected = jnp.zeros(resid_in.shape, jnp.float32)
    for part_index in range(N_TP):
        low_n = part_index * narrow_cols
        low_w = part_index * wide_cols
        partial_value = jnp.dot(att_narrow[:, low_n:low_n + narrow_cols], out_narrow[low_n:low_n + narrow_cols], preferred_element_type=jnp.float32)
        partial_value = partial_value + jnp.dot(att_wide[:, low_w:low_w + wide_cols], out_wide[low_w:low_w + wide_cols], preferred_element_type=jnp.float32)
        projected = rounded_add(projected, partial_value)
    middle = (resid_in.astype(jnp.float32) + projected).astype(jnp.bfloat16)
    middle_f32 = middle.astype(jnp.float32)
    normed = middle_f32 * lax.rsqrt(lax.optimization_barrier(jnp.mean(middle_f32 * middle_f32, axis=-1, keepdims=True)) + NORM_EPS)
    normed = (normed * norm_gain.astype(jnp.float32)).astype(jnp.bfloat16)
    hidden_cols = up_weight.shape[1] // N_TP
    mixer = jnp.zeros(resid_in.shape, jnp.float32)
    for part_index in range(N_TP):
        low_h = part_index * hidden_cols
        lifted = jnp.dot(normed, up_weight[:, low_h:low_h + hidden_cols], preferred_element_type=jnp.float32)
        activated = jnp.square(jax.nn.relu(lifted)).astype(jnp.bfloat16)
        partial_value = jnp.dot(activated, down_weight[low_h:low_h + hidden_cols], preferred_element_type=jnp.float32)
        mixer = rounded_add(mixer, partial_value)
    return (middle_f32 + mixer).astype(jnp.bfloat16)
```

```python
import math

import jax
import jax.numpy as jnp
from jax import lax
from jax.experimental import pallas as pl
from jax.experimental.pallas import tpu as pltpu
from jax.sharding import PartitionSpec as P

NORM_EPS = 1e-06
OUT_SCALE = 0.8


def empty_state(query, key_head_stack, value_width):
    row_count, head_count = (query.shape[0], query.shape[1])
    group_size = head_count // key_head_stack
    row_top = jnp.full((key_head_stack, group_size, 2, row_count), -jnp.inf, jnp.float32)
    row_total = jnp.zeros((key_head_stack, group_size, 2, row_count), jnp.float32)
    weighted_values = jnp.zeros(
        (key_head_stack, group_size, 2, row_count, value_width), jnp.float32
    )
    return (row_top, row_total, weighted_values)


def absorb(states, query, key_rows, values):
    row_count, head_count = (query.shape[0], query.shape[1])
    key_head_stack = key_rows.shape[1]
    half_width = key_rows.shape[2] // 2
    group_size = head_count // key_head_stack
    value_width = values.shape[2]
    amount = key_rows.shape[0]
    block_rows = math.gcd(amount, 512)
    rotation_count = amount // block_rows
    grouped = query.reshape(row_count, key_head_stack, group_size, 2, half_width)
    key_block_list = key_rows.reshape(rotation_count, block_rows, key_head_stack, 2, half_width)
    value_blocks = values.reshape(rotation_count, block_rows, key_head_stack, value_width)

    def visit(running, kv_pair):
        row_top, row_total, weighted_values = running
        key_blk, value_blk = kv_pair
        scores = jnp.einsum(
            "tkgcd,skcd->kgcts", grouped, key_blk, preferred_element_type=jnp.float32
        ) * half_width ** (-0.5)
        new_top = jnp.maximum(row_top, jnp.max(scores, axis=-1))
        rescale = jnp.exp(row_top - new_top)
        powers = jnp.exp(scores - new_top[..., None])
        row_total = row_total * rescale + jnp.sum(powers, axis=-1)
        weighted_values = weighted_values * rescale[..., None] + jnp.einsum(
            "iodph,hie->iodpe",
            powers.astype(jnp.bfloat16),
            value_blk,
            preferred_element_type=jnp.float32,
        )
        return ((new_top, row_total, weighted_values), None)

    outcome, _ = lax.scan(visit, states, (key_block_list, value_blocks))
    return outcome


def finish(states, lambdas, gain_vec):
    row_top, row_total, weighted_values = states
    key_head_stack, group_size, row_count = (row_top.shape[0], row_top.shape[1], row_top.shape[3])
    value_width = weighted_values.shape[4]
    first_map = weighted_values[:, :, 0] / row_total[:, :, 0, :, None]
    second_map = weighted_values[:, :, 1] / row_total[:, :, 1, :, None]
    mixed = first_map - lambdas.reshape(key_head_stack, group_size)[:, :, None, None] * second_map
    normed = (
        mixed
        * lax.rsqrt(jnp.mean(mixed * mixed, axis=-1, keepdims=True) + NORM_EPS)
        * gain_vec
        * OUT_SCALE
    )
    normed = normed.astype(jnp.bfloat16).transpose(2, 0, 1, 3)
    return normed.reshape(row_count, key_head_stack * group_size * value_width)


def attend(
    query_narrow,
    key_narrow,
    value_narrow,
    query_wide,
    key_wide,
    value_wide,
    lambda_narrow,
    lambda_wide,
    head_gain,
):
    initial = (
        empty_state(query_narrow, key_narrow.shape[1], value_narrow.shape[2]),
        empty_state(query_wide, key_wide.shape[1], value_wide.shape[2]),
    )
    narrow_keys = lax.all_gather(key_narrow, "sp", axis=0, tiled=True)
    narrow_values = lax.all_gather(value_narrow, "sp", axis=0, tiled=True)
    wide_keys = lax.all_gather(key_wide, "sp", axis=0, tiled=True)
    wide_values = lax.all_gather(value_wide, "sp", axis=0, tiled=True)
    narrow_state = absorb(initial[0], query_narrow, narrow_keys, narrow_values)
    wide_state = absorb(initial[1], query_wide, wide_keys, wide_values)
    return (
        finish(narrow_state, lambda_narrow, head_gain),
        finish(wide_state, lambda_wide, head_gain),
    )


def shards(
    resid_in,
    query_narrow,
    key_narrow,
    value_narrow,
    query_wide,
    key_wide,
    value_wide,
    lambda_narrow,
    lambda_wide,
    head_gain,
    out_narrow,
    out_wide,
    norm_gain,
    up_weight,
    down_weight,
):
    att_narrow, att_wide = attend(
        query_narrow,
        key_narrow,
        value_narrow,
        query_wide,
        key_wide,
        value_wide,
        lambda_narrow,
        lambda_wide,
        head_gain,
    )
    projected = lax.psum_scatter(
        (
            jnp.dot(att_narrow, out_narrow, preferred_element_type=jnp.float32)
            + jnp.dot(att_wide, out_wide, preferred_element_type=jnp.float32)
        ).astype(jnp.bfloat16),
        "tp",
        scatter_dimension=0,
        tiled=True,
    ).astype(jnp.float32)
    middle = (resid_in.astype(jnp.float32) + projected).astype(jnp.bfloat16)
    middle_f32 = middle.astype(jnp.float32)
    normed = middle_f32 * lax.rsqrt(
        jnp.mean(middle_f32 * middle_f32, axis=-1, keepdims=True) + NORM_EPS
    )
    normed = (normed * norm_gain.astype(jnp.float32)).astype(jnp.bfloat16)
    whole_rows = lax.all_gather(normed, "tp", axis=0, tiled=True)
    up_collected = lax.all_gather(up_weight, "sp", axis=0, tiled=True)
    lifted = jnp.dot(whole_rows, up_collected, preferred_element_type=jnp.float32)
    activated = jnp.square(jax.nn.relu(lifted)).astype(jnp.bfloat16)
    partials = jnp.dot(
        activated,
        lax.all_gather(down_weight, "sp", axis=1, tiled=True),
        preferred_element_type=jnp.float32,
    )
    mixer_out = lax.psum_scatter(
        partials.astype(jnp.bfloat16), "tp", scatter_dimension=0, tiled=True
    ).astype(jnp.float32)
    return (middle_f32 + mixer_out).astype(jnp.bfloat16)


LOG2E = math.log2(math.e)
VMEM_BYTES = 60 * 2**20


def dot32(a, b):
    return jnp.dot(a, b, preferred_element_type=jnp.float32)


def layer_kernel(plan, resid, q, kv, lam_n, lam_w, head_gain, out_n, out_w, norm_gain, up, down,
                 out, kv_full, att, proj_send, proj_recv, middle, act, up_full, down_full,
                 part, core_recv, x_send, x_recv, z_send, z_recv, total,
                 kv_ss, kv_rs, wz_ss, wz_rs, wy_ss, wy_rs, wl_sem, p_ss, p_rs,
                 az_ss, az_rs, ax_ss, ax_rs, ac_ss, ac_rs,
                 rc_ss, rc_rs, rx_ss, rx_rs, rz_ss, rz_rs):
    grp_n, sp_n, tp_n, maps = plan
    g, s, t = lax.axis_index("grp"), lax.axis_index("sp"), lax.axis_index("tp")
    rows = kv.shape[0]
    mine = resid.shape[0]
    width = resid.shape[1]
    deep = up.shape[0]
    hid = up_full.shape[1]
    f32, bf16 = jnp.float32, jnp.bfloat16

    def ahead(d):
        return lax.rem(s + d, sp_n)

    def behind(d):
        return lax.rem(s + sp_n - d, sp_n)

    x_peer = lax.rem(t + 2, tp_n)
    c_peer = t + 1 - 2 * lax.rem(t, 2)
    y_peer = 1 - g

    def send(src, dst, ss, rs, dev):
        copy = pltpu.make_async_remote_copy(
            src_ref=src, dst_ref=dst, send_sem=ss, recv_sem=rs,
            device_id=dev, device_id_type=pl.DeviceIdType.MESH)
        return copy

    barrier = pltpu.get_barrier_semaphore()
    peers = [{"sp": ahead(d)} for d in range(1, sp_n)]
    peers += [{"tp": lax.rem(t + d, tp_n)} for d in range(1, tp_n)]
    peers += [{"grp": y_peer}]
    for peer in peers:
        pl.semaphore_signal(barrier, inc=1, device_id=peer, device_id_type=pl.DeviceIdType.MESH)
    pl.semaphore_wait(barrier, len(peers))

    kv_copy = []
    for d in range(1, sp_n):
        copy = send(kv, kv_full.at[pl.ds(s * rows, rows)], kv_ss.at[d], kv_rs.at[d], {"sp": ahead(d)})
        copy.start()
        kv_copy.append(copy)

    half_d, half_h = deep // grp_n, hid // grp_n
    wz = []
    for d in range(1, sp_n):
        to = ahead(d)
        pair = (
            send(up.at[pl.ds(g * half_d, half_d), pl.ds(pl.multiple_of(to * hid, 128), hid)],
                 up_full.at[pl.ds(s * deep + g * half_d, half_d)],
                 wz_ss.at[0, d], wz_rs.at[0, d], {"sp": to}),
            send(down.at[pl.ds(to * hid + g * half_h, half_h)],
                 down_full.at[pl.ds(g * half_h, half_h), pl.ds(pl.multiple_of(s * deep, 128), deep)],
                 wz_ss.at[1, d], wz_rs.at[1, d], {"sp": to}),
        )
        for copy in pair:
            copy.start()
        wz.append(pair)
    own_up = pltpu.make_async_copy(
        up.at[:, pl.ds(pl.multiple_of(s * hid, 128), hid)], up_full.at[pl.ds(s * deep, deep)], wl_sem.at[0])
    own_down = pltpu.make_async_copy(
        down.at[pl.ds(s * hid, hid)], down_full.at[:, pl.ds(pl.multiple_of(s * deep, 128), deep)], wl_sem.at[1])
    own_up.start()
    own_down.start()

    kv_full[pl.ds(s * rows, rows)] = kv[...]
    for copy in kv_copy:
        copy.wait_recv()

    for h, (pair, lam_of, v_at, scale) in enumerate(maps):
        lam = (lam_n if lam_of[0] == 0 else lam_w)[lam_of[1]]
        sides = []
        for q_at, k_at, k_width in pair:
            scores = lax.dot_general(
                q[:, q_at:q_at + k_width], kv_full[:, k_at:k_at + k_width],
                (((1,), (1,)), ((), ())), preferred_element_type=f32)
            top = jnp.max(scores, axis=-1, keepdims=True)
            powers = jnp.exp2((scores - top) * (scale * LOG2E))
            row_total = jnp.sum(powers, axis=-1, keepdims=True)
            vals = kv_full[:, v_at:v_at + head_gain.shape[1]]
            sides.append(dot32(powers.astype(bf16), vals) / row_total)
        mixed = sides[0] - lam * sides[1]
        v_width = mixed.shape[1]
        normed = (mixed * lax.rsqrt(jnp.mean(mixed * mixed, axis=-1, keepdims=True) + NORM_EPS)
                  * head_gain[...] * OUT_SCALE)
        att[:, h * v_width:(h + 1) * v_width] = normed.astype(bf16)

    cut = out_n.shape[0]
    chunk = math.gcd(width, 512)

    @pl.loop(0, width // chunk)
    def _(j):
        cols = pl.ds(pl.multiple_of(j * chunk, chunk), chunk)
        proj_send[:, cols] = (dot32(att[:, :cut], out_n[:, cols]) + dot32(att[:, cut:], out_w[:, cols])).astype(bf16)

    p_copy = []
    for d in (2, 3, 1):
        to = lax.rem(t + d, tp_n)
        copy = send(proj_send.at[pl.ds(to * mine, mine)], proj_recv.at[d], p_ss.at[d], p_rs.at[d], {"tp": to})
        copy.start()
        p_copy.append(copy)

    wy = []

    def forward_weights(d):
        for copy in wz[d - 1]:
            copy.wait_recv()
        at = behind(d)
        a = up_full.at[pl.ds(at * deep + g * half_d, half_d)]
        b = down_full.at[pl.ds(g * half_h, half_h), pl.ds(pl.multiple_of(at * deep, 128), deep)]
        for kind, ref in enumerate((a, b)):
            copy = send(ref, ref, wy_ss.at[kind, d], wy_rs.at[kind, d], {"grp": y_peer})
            copy.start()
            wy.append(copy)

    forward_weights(1)
    for copy in p_copy:
        copy.wait_recv()
    projected = proj_send[pl.ds(t * mine, mine)].astype(f32)
    for d in range(1, tp_n):
        projected = projected + proj_recv[d].astype(f32)
    mid = (resid[...].astype(f32) + projected).astype(bf16)
    middle[...] = mid
    mid32 = mid.astype(f32)
    normed = mid32 * lax.rsqrt(jnp.mean(mid32 * mid32, axis=-1, keepdims=True) + NORM_EPS)

    def block(z, who):
        return act.at[pl.ds(z * rows + who * mine, mine)]

    act[pl.ds(s * rows + t * mine, mine)] = (normed * norm_gain[...].astype(f32)).astype(bf16)

    az, ax, ac = [], [], []
    for d in range(1, sp_n):
        copy = send(block(s, t), block(s, t), az_ss.at[d], az_rs.at[d], {"sp": ahead(d)})
        copy.start()
        az.append(copy)

    def spread(d):
        if d:
            az[d - 1].wait_recv()
        ref = block(behind(d), t)
        a = send(ref, ref, ax_ss.at[d], ax_rs.at[d], {"tp": x_peer})
        a.start()
        ax.append(a)
        c = send(ref, ref, ac_ss.at[0, d], ac_rs.at[0, d], {"tp": c_peer})
        c.start()
        ac.append([c])

    spread(0)
    for d in range(2, sp_n):
        forward_weights(d)
    own_up.wait()
    own_down.wait()
    for copy in wy:
        copy.wait_recv()

    rc, rx, rz = [], [], []

    def compute(d):
        ax[d].wait_recv()
        ref = block(behind(d), x_peer)
        c = send(ref, ref, ac_ss.at[1, d], ac_rs.at[1, d], {"tp": c_peer})
        c.start()
        ac[d].append(c)
        if d + 1 < sp_n:
            spread(d + 1)
        for copy in ac[d]:
            copy.wait_recv()
        lifted = dot32(act[pl.ds(behind(d) * rows, rows)], up_full[...])
        hidden = jnp.square(jnp.maximum(lifted, 0.0)).astype(bf16)

        @pl.loop(0, width // chunk)
        def _(j):
            cols = pl.ds(pl.multiple_of(j * chunk, chunk), chunk)
            part[d, :, cols] = dot32(hidden, down_full[:, cols]).astype(bf16)

        pair = []
        for i, who in enumerate((c_peer, lax.rem(c_peer + 2, tp_n))):
            copy = send(part.at[d, pl.ds(who * mine, mine)], core_recv.at[d, i], rc_ss.at[d, i], rc_rs.at[d, i],
                        {"tp": c_peer})
            copy.start()
            pair.append(copy)
        rc.append(pair)

    def across(d):
        for copy in rc[d]:
            copy.wait_recv()
        x_send[d] = (part[d, pl.ds(x_peer * mine, mine)].astype(f32) + core_recv[d, 1].astype(f32)).astype(bf16)
        copy = send(x_send.at[d], x_recv.at[d], rx_ss.at[d], rx_rs.at[d], {"tp": x_peer})
        copy.start()
        rx.append(copy)

    def home(d):
        rx[d].wait_recv()
        term = (part[d, pl.ds(t * mine, mine)].astype(f32) + core_recv[d, 0].astype(f32)
                + x_recv[d].astype(f32))
        if d == 0:
            total[...] = term
            return
        z_send[d] = term.astype(bf16)
        copy = send(z_send.at[d], z_recv.at[d], rz_ss.at[d], rz_rs.at[d], {"sp": behind(d)})
        copy.start()
        rz.append(copy)

    for step in range(sp_n + 2):
        if step < sp_n:
            compute(step)
        if 0 <= step - 1 < sp_n:
            across(step - 1)
        if 0 <= step - 2 < sp_n:
            home(step - 2)
    mixer = total[...]
    for copy in rz:
        copy.wait_recv()
    for d in range(1, sp_n):
        mixer = mixer + z_recv[d].astype(f32)
    out[...] = (middle[...].astype(f32) + mixer).astype(bf16)
    sent = kv_copy + [c for pair in wz for c in pair] + p_copy + wy + az + ax
    sent += [c for pair in ac for c in pair] + [c for pair in rc for c in pair] + rx + rz
    for copy in sent:
        copy.wait_send()


def split_maps(query, masked):
    row_count, heads, both = query.shape
    half = both // 2
    if not masked:
        return query.reshape(row_count, heads * both)
    zero = jnp.zeros_like(query[:, :, :half])
    first = jnp.concatenate([query[:, :, :half], zero], axis=-1)
    second = jnp.concatenate([zero, query[:, :, half:]], axis=-1)
    return jnp.stack([first, second], axis=2).reshape(row_count, heads * 2 * both)


def fused(sizes, resid_in, query_narrow, key_narrow, value_narrow, query_wide, key_wide, value_wide,
          lambda_narrow, lambda_wide, head_gain, out_narrow, out_wide, norm_gain, up_weight, down_weight):
    grp_n, sp_n, tp_n = sizes
    bf16, f32 = jnp.bfloat16, jnp.float32
    q_parts, kv_parts, maps = [], [], []
    q_at = kv_at = 0
    for kind, (query, key, value) in enumerate(
            ((query_narrow, key_narrow, value_narrow), (query_wide, key_wide, value_wide))):
        rows, heads, both = query.shape
        kheads, v_width = key.shape[1], value.shape[2]
        half = both // 2
        masked = half % 128 != 0
        q_parts.append(split_maps(query, masked))
        kv_parts += [key.reshape(rows, kheads * both), value.reshape(rows, kheads * v_width)]
        for h in range(heads):
            kh = h // (heads // kheads)
            k0 = kv_at + kh * both
            v0 = kv_at + kheads * both + kh * v_width
            if masked:
                pair = tuple((q_at + (2 * h + c) * both, k0, both) for c in range(2))
            else:
                pair = tuple((q_at + h * both + c * half, k0 + c * half, half) for c in range(2))
            maps.append((pair, (kind, h), v0, half ** -0.5))
        q_at += q_parts[-1].shape[1]
        kv_at += kheads * (both + v_width)
    q = jnp.concatenate(q_parts, axis=1)
    kv = jnp.concatenate(kv_parts, axis=1)
    mine, width = resid_in.shape
    deep, hid = up_weight.shape[0], up_weight.shape[1] // sp_n
    vm, sm, anyw = (pl.BlockSpec(memory_space=m) for m in (pltpu.VMEM, pltpu.SMEM, pl.ANY))
    dma = pltpu.SemaphoreType.DMA
    n = sp_n
    scratch = [
        pltpu.VMEM((n * rows, kv.shape[1]), bf16),
        pltpu.VMEM((rows, len(maps) * v_width), bf16),
        pltpu.VMEM((rows, width), bf16),
        pltpu.VMEM((tp_n, mine, width), bf16),
        pltpu.VMEM((mine, width), bf16),
        pltpu.VMEM((n * rows, width), bf16),
        pltpu.VMEM((width, hid), bf16),
        pltpu.VMEM((hid, width), bf16),
        pltpu.VMEM((n, rows, width), bf16),
        pltpu.VMEM((n, 2, mine, width), bf16),
        pltpu.VMEM((n, mine, width), bf16),
        pltpu.VMEM((n, mine, width), bf16),
        pltpu.VMEM((n, mine, width), bf16),
        pltpu.VMEM((n, mine, width), bf16),
        pltpu.VMEM((mine, width), f32),
        dma((n,)), dma((n,)),
        dma((2, n)), dma((2, n)), dma((2, n)), dma((2, n)), dma((2,)),
        dma((tp_n,)), dma((tp_n,)),
        dma((n,)), dma((n,)), dma((n,)), dma((n,)), dma((2, n)), dma((2, n)),
        dma((n, 2)), dma((n, 2)), dma((n,)), dma((n,)), dma((n,)), dma((n,)),
    ]
    return pl.pallas_call(
        lambda *refs: layer_kernel((grp_n, sp_n, tp_n, tuple(maps)), *refs),
        out_shape=jax.ShapeDtypeStruct(resid_in.shape, bf16),
        in_specs=[vm, vm, vm, sm, sm, vm, vm, vm, vm, anyw, anyw],
        out_specs=vm,
        scratch_shapes=scratch,
        compiler_params=pltpu.CompilerParams(
            collective_id=0, has_side_effects=True, vmem_limit_bytes=VMEM_BYTES),
        name="layer",
    )(resid_in, q, kv, lambda_narrow, lambda_wide, head_gain[None], out_narrow, out_wide,
      norm_gain[None], up_weight, down_weight)


def fits(sizes, resid_in, query_narrow, up_weight):
    grp_n, sp_n, tp_n = sizes
    rows, width = query_narrow.shape[0], resid_in.shape[1]
    held = 2 * width * (3 * sp_n * rows + 2 * rows + 2 * up_weight.shape[1] // sp_n)
    return (grp_n == 2 and tp_n == 4 and up_weight.shape[1] % (sp_n * 256) == 0
            and up_weight.shape[0] % 256 == 0 and held < VMEM_BYTES // 2)


def solution(mesh):
    placed = (
        P(("grp", "sp", "tp"), None),
        P(("grp", "sp"), "tp", None),
        P(("grp", "sp"), "tp", None),
        P(("grp", "sp"), "tp", None),
        P(("grp", "sp"), "tp", None),
        P(("grp", "sp"), "tp", None),
        P(("grp", "sp"), "tp", None),
        P("tp"),
        P("tp"),
        P(),
        P("tp", None),
        P("tp", None),
        P(),
        P("sp", "tp"),
        P("tp", "sp"),
    )
    sizes = tuple(mesh.shape[axis] for axis in ("grp", "sp", "tp"))

    def layer(*blocks):
        if fits(sizes, blocks[0], blocks[1], blocks[13]):
            return fused(sizes, *blocks)
        return shards(*blocks)

    return jax.shard_map(
        layer, mesh=mesh, in_specs=placed, out_specs=P(("grp", "sp", "tp"), None), check_vma=False
    )
```

```python
import math

import jax
import jax.numpy as jnp
from jax import lax
from jax.experimental import pallas as pl
from jax.experimental.pallas import tpu as pltpu
from jax.sharding import PartitionSpec as P

NORM_EPS = 1e-06
OUT_SCALE = 0.8


def empty_state(query, key_head_stack, value_width):
    row_count, head_count = (query.shape[0], query.shape[1])
    group_size = head_count // key_head_stack
    row_top = jnp.full((key_head_stack, group_size, 2, row_count), -jnp.inf, jnp.float32)
    row_total = jnp.zeros((key_head_stack, group_size, 2, row_count), jnp.float32)
    weighted_values = jnp.zeros(
        (key_head_stack, group_size, 2, row_count, value_width), jnp.float32
    )
    return (row_top, row_total, weighted_values)


def absorb(states, query, key_rows, values):
    row_count, head_count = (query.shape[0], query.shape[1])
    key_head_stack = key_rows.shape[1]
    half_width = key_rows.shape[2] // 2
    group_size = head_count // key_head_stack
    value_width = values.shape[2]
    amount = key_rows.shape[0]
    block_rows = math.gcd(amount, 512)
    rotation_count = amount // block_rows
    grouped = query.reshape(row_count, key_head_stack, group_size, 2, half_width)
    key_block_list = key_rows.reshape(rotation_count, block_rows, key_head_stack, 2, half_width)
    value_blocks = values.reshape(rotation_count, block_rows, key_head_stack, value_width)

    def visit(running, kv_pair):
        row_top, row_total, weighted_values = running
        key_blk, value_blk = kv_pair
        scores = jnp.einsum(
            "tkgcd,skcd->kgcts", grouped, key_blk, preferred_element_type=jnp.float32
        ) * half_width ** (-0.5)
        new_top = jnp.maximum(row_top, jnp.max(scores, axis=-1))
        rescale = jnp.exp(row_top - new_top)
        powers = jnp.exp(scores - new_top[..., None])
        row_total = row_total * rescale + jnp.sum(powers, axis=-1)
        weighted_values = weighted_values * rescale[..., None] + jnp.einsum(
            "iodph,hie->iodpe",
            powers.astype(jnp.bfloat16),
            value_blk,
            preferred_element_type=jnp.float32,
        )
        return ((new_top, row_total, weighted_values), None)

    outcome, _ = lax.scan(visit, states, (key_block_list, value_blocks))
    return outcome


def finish(states, lambdas, gain_vec):
    row_top, row_total, weighted_values = states
    key_head_stack, group_size, row_count = (row_top.shape[0], row_top.shape[1], row_top.shape[3])
    value_width = weighted_values.shape[4]
    first_map = weighted_values[:, :, 0] / row_total[:, :, 0, :, None]
    second_map = weighted_values[:, :, 1] / row_total[:, :, 1, :, None]
    mixed = first_map - lambdas.reshape(key_head_stack, group_size)[:, :, None, None] * second_map
    normed = (
        mixed
        * lax.rsqrt(jnp.mean(mixed * mixed, axis=-1, keepdims=True) + NORM_EPS)
        * gain_vec
        * OUT_SCALE
    )
    normed = normed.astype(jnp.bfloat16).transpose(2, 0, 1, 3)
    return normed.reshape(row_count, key_head_stack * group_size * value_width)


def attend(
    query_narrow,
    key_narrow,
    value_narrow,
    query_wide,
    key_wide,
    value_wide,
    lambda_narrow,
    lambda_wide,
    head_gain,
):
    initial = (
        empty_state(query_narrow, key_narrow.shape[1], value_narrow.shape[2]),
        empty_state(query_wide, key_wide.shape[1], value_wide.shape[2]),
    )
    narrow_keys = lax.all_gather(key_narrow, "sp", axis=0, tiled=True)
    narrow_values = lax.all_gather(value_narrow, "sp", axis=0, tiled=True)
    wide_keys = lax.all_gather(key_wide, "sp", axis=0, tiled=True)
    wide_values = lax.all_gather(value_wide, "sp", axis=0, tiled=True)
    narrow_state = absorb(initial[0], query_narrow, narrow_keys, narrow_values)
    wide_state = absorb(initial[1], query_wide, wide_keys, wide_values)
    return (
        finish(narrow_state, lambda_narrow, head_gain),
        finish(wide_state, lambda_wide, head_gain),
    )


def shards(
    resid_in,
    query_narrow,
    key_narrow,
    value_narrow,
    query_wide,
    key_wide,
    value_wide,
    lambda_narrow,
    lambda_wide,
    head_gain,
    out_narrow,
    out_wide,
    norm_gain,
    up_weight,
    down_weight,
):
    att_narrow, att_wide = attend(
        query_narrow,
        key_narrow,
        value_narrow,
        query_wide,
        key_wide,
        value_wide,
        lambda_narrow,
        lambda_wide,
        head_gain,
    )
    projected = lax.psum_scatter(
        (
            jnp.dot(att_narrow, out_narrow, preferred_element_type=jnp.float32)
            + jnp.dot(att_wide, out_wide, preferred_element_type=jnp.float32)
        ).astype(jnp.bfloat16),
        "tp",
        scatter_dimension=0,
        tiled=True,
    ).astype(jnp.float32)
    middle = (resid_in.astype(jnp.float32) + projected).astype(jnp.bfloat16)
    middle_f32 = middle.astype(jnp.float32)
    normed = middle_f32 * lax.rsqrt(
        jnp.mean(middle_f32 * middle_f32, axis=-1, keepdims=True) + NORM_EPS
    )
    normed = (normed * norm_gain.astype(jnp.float32)).astype(jnp.bfloat16)
    whole_rows = lax.all_gather(normed, "tp", axis=0, tiled=True)
    up_collected = lax.all_gather(up_weight, "sp", axis=0, tiled=True)
    lifted = jnp.dot(whole_rows, up_collected, preferred_element_type=jnp.float32)
    activated = jnp.square(jax.nn.relu(lifted)).astype(jnp.bfloat16)
    partials = jnp.dot(
        activated,
        lax.all_gather(down_weight, "sp", axis=1, tiled=True),
        preferred_element_type=jnp.float32,
    )
    mixer_out = lax.psum_scatter(
        partials.astype(jnp.bfloat16), "tp", scatter_dimension=0, tiled=True
    ).astype(jnp.float32)
    return (middle_f32 + mixer_out).astype(jnp.bfloat16)


LOG2E = math.log2(math.e)
VMEM_BYTES = 60 * 2**20


def dot32(a, b):
    return jnp.dot(a, b, preferred_element_type=jnp.float32)


def layer_kernel(plan, resid, q, kv, lam_n, lam_w, head_gain, out_n, out_w, norm_gain, up, down,
                 out, kv_full, att, proj_send, proj_recv, middle, act, up_full, down_full,
                 part, core_recv, x_send, x_recv, z_send, z_recv, total,
                 kv_ss, kv_rs, wz_ss, wz_rs, wy_ss, wy_rs, wl_sem, p_ss, p_rs,
                 az_ss, az_rs, ax_ss, ax_rs, ac_ss, ac_rs,
                 rc_ss, rc_rs, rx_ss, rx_rs, rz_ss, rz_rs):
    grp_n, sp_n, tp_n, maps = plan
    g, s, t = lax.axis_index("grp"), lax.axis_index("sp"), lax.axis_index("tp")
    rows = kv.shape[0]
    mine = resid.shape[0]
    width = resid.shape[1]
    deep = up.shape[0]
    hid = up_full.shape[1]
    f32, bf16 = jnp.float32, jnp.bfloat16

    def ahead(d):
        return lax.rem(s + d, sp_n)

    def behind(d):
        return lax.rem(s + sp_n - d, sp_n)

    x_peer = lax.rem(t + 2, tp_n)
    c_peer = t + 1 - 2 * lax.rem(t, 2)
    y_peer = 1 - g

    def send(src, dst, ss, rs, dev):
        copy = pltpu.make_async_remote_copy(
            src_ref=src, dst_ref=dst, send_sem=ss, recv_sem=rs,
            device_id=dev, device_id_type=pl.DeviceIdType.MESH)
        return copy

    barrier = pltpu.get_barrier_semaphore()
    peers = [{"sp": ahead(d)} for d in range(1, sp_n)]
    peers += [{"tp": lax.rem(t + d, tp_n)} for d in range(1, tp_n)]
    peers += [{"grp": y_peer}]
    for peer in peers:
        pl.semaphore_signal(barrier, inc=1, device_id=peer, device_id_type=pl.DeviceIdType.MESH)
    pl.semaphore_wait(barrier, len(peers))

    half_d, half_h = deep // grp_n, hid // grp_n
    wz = []
    for d in range(1, sp_n):
        to = ahead(d)
        pair = (
            send(up.at[pl.ds(g * half_d, half_d), pl.ds(pl.multiple_of(to * hid, 128), hid)],
                 up_full.at[pl.ds(s * deep + g * half_d, half_d)],
                 wz_ss.at[0, d], wz_rs.at[0, d], {"sp": to}),
            send(down.at[pl.ds(to * hid + g * half_h, half_h)],
                 down_full.at[pl.ds(g * half_h, half_h), pl.ds(pl.multiple_of(s * deep, 128), deep)],
                 wz_ss.at[1, d], wz_rs.at[1, d], {"sp": to}),
        )
        wz.append(pair)
    own_up = pltpu.make_async_copy(
        up.at[:, pl.ds(pl.multiple_of(s * hid, 128), hid)], up_full.at[pl.ds(s * deep, deep)], wl_sem.at[0])
    own_down = pltpu.make_async_copy(
        down.at[pl.ds(s * hid, hid)], down_full.at[:, pl.ds(pl.multiple_of(s * deep, 128), deep)], wl_sem.at[1])
    own_up.start()
    own_down.start()

    def passing(k, way):
        at = pl.ds((s - way * k) * rows, rows)
        lane = (1 - way) // 2
        return send(kv if k == 0 else kv_full.at[at], kv_full.at[at], kv_ss.at[lane, k], kv_rs.at[lane, k],
                    {"sp": s + way})

    def arriving(k, way):
        at = pl.ds((s - way * k) * rows, rows)
        lane = (1 - way) // 2
        return send(kv, kv_full.at[at], kv_ss.at[lane, k - 1], kv_rs.at[lane, k - 1], {"sp": s})

    def passes(k, way):
        return (s >= k) & (s < sp_n - 1) if way == 1 else (s <= sp_n - 1 - k) & (s > 0)

    for k in range(sp_n):
        for way in (1, -1):
            @pl.when((s >= k) if way == 1 else (s <= sp_n - 1 - k))
            def _():
                if k:
                    arriving(k, way).wait_recv()

            @pl.when(passes(k, way))
            def _():
                passing(k, way).start()

        @pl.when(s == k)
        def _():
            for d in range(1, sp_n - k):
                for copy in wz[d - 1]:
                    copy.start()

        @pl.when(s == sp_n - 1 - k)
        def _():
            for d in range(k + 1, sp_n):
                for copy in wz[d - 1]:
                    copy.start()

        if k == 0:
            kv_full[pl.ds(s * rows, rows)] = kv[...]

    for h, (pair, lam_of, v_at, scale) in enumerate(maps):
        lam = (lam_n if lam_of[0] == 0 else lam_w)[lam_of[1]]
        sides = []
        for q_at, k_at, k_width in pair:
            scores = lax.dot_general(
                q[:, q_at:q_at + k_width], kv_full[:, k_at:k_at + k_width],
                (((1,), (1,)), ((), ())), preferred_element_type=f32)
            top = jnp.max(scores, axis=-1, keepdims=True)
            powers = jnp.exp2((scores - top) * (scale * LOG2E))
            row_total = jnp.sum(powers, axis=-1, keepdims=True)
            vals = kv_full[:, v_at:v_at + head_gain.shape[1]]
            sides.append(dot32(powers.astype(bf16), vals) / row_total)
        mixed = sides[0] - lam * sides[1]
        v_width = mixed.shape[1]
        normed = (mixed * lax.rsqrt(jnp.mean(mixed * mixed, axis=-1, keepdims=True) + NORM_EPS)
                  * head_gain[...] * OUT_SCALE)
        att[:, h * v_width:(h + 1) * v_width] = normed.astype(bf16)

    cut = out_n.shape[0]
    chunk = math.gcd(width, 512)

    @pl.loop(0, width // chunk)
    def _(j):
        cols = pl.ds(pl.multiple_of(j * chunk, chunk), chunk)
        proj_send[:, cols] = (dot32(att[:, :cut], out_n[:, cols]) + dot32(att[:, cut:], out_w[:, cols])).astype(bf16)

    p_copy = []
    for d in (2, 3, 1):
        to = lax.rem(t + d, tp_n)
        copy = send(proj_send.at[pl.ds(to * mine, mine)], proj_recv.at[d], p_ss.at[d], p_rs.at[d], {"tp": to})
        copy.start()
        p_copy.append(copy)

    wy = []

    def forward_weights(d):
        for copy in wz[d - 1]:
            copy.wait_recv()
        at = behind(d)
        a = up_full.at[pl.ds(at * deep + g * half_d, half_d)]
        b = down_full.at[pl.ds(g * half_h, half_h), pl.ds(pl.multiple_of(at * deep, 128), deep)]
        for kind, ref in enumerate((a, b)):
            copy = send(ref, ref, wy_ss.at[kind, d], wy_rs.at[kind, d], {"grp": y_peer})
            copy.start()
            wy.append(copy)

    for d in range(1, sp_n - 1):
        forward_weights(d)
    for copy in p_copy:
        copy.wait_recv()
    projected = proj_send[pl.ds(t * mine, mine)].astype(f32)
    for d in range(1, tp_n):
        projected = projected + proj_recv[d].astype(f32)
    mid = (resid[...].astype(f32) + projected).astype(bf16)
    middle[...] = mid
    mid32 = mid.astype(f32)
    normed = mid32 * lax.rsqrt(jnp.mean(mid32 * mid32, axis=-1, keepdims=True) + NORM_EPS)

    half_rows, half_mine = rows // 2, mine // 2
    parts = 2 * sp_n

    def group(z, half):
        return (2 * z + half) * half_rows

    def block(z, half, who):
        return act.at[pl.ds(group(z, half) + who * half_mine, half_mine)]

    sealed = (normed * norm_gain[...].astype(f32)).astype(bf16)
    for half in range(2):
        act[pl.ds(group(s, half) + t * half_mine, half_mine)] = sealed[half * half_mine:(half + 1) * half_mine]

    az, ax, ac = {}, {}, {}
    for b in range(2, parts):
        ref = block(s, b % 2, t)
        az[b] = send(ref, ref, az_ss.at[b], az_rs.at[b], {"sp": ahead(b // 2)})
        az[b].start()

    def spread(b):
        if b >= parts:
            return
        if b >= 2:
            az[b].wait_recv()
        ref = block(behind(b // 2), b % 2, t)
        ax[b] = send(ref, ref, ax_ss.at[b], ax_rs.at[b], {"tp": x_peer})
        ax[b].start()
        ac[b] = [send(ref, ref, ac_ss.at[0, b], ac_rs.at[0, b], {"tp": c_peer})]
        ac[b][0].start()

    def cross(b):
        if b >= parts:
            return
        ax[b].wait_recv()
        ref = block(behind(b // 2), b % 2, x_peer)
        copy = send(ref, ref, ac_ss.at[1, b], ac_rs.at[1, b], {"tp": c_peer})
        copy.start()
        ac[b].append(copy)

    rc, rx, rz = {}, {}, []

    def compute(b):
        for copy in ac[b]:
            copy.wait_recv()
        lifted = dot32(act[pl.ds(group(behind(b // 2), b % 2), half_rows)], up_full[...])
        hidden = jnp.square(jnp.maximum(lifted, 0.0)).astype(bf16)

        @pl.loop(0, width // chunk)
        def _(j):
            cols = pl.ds(pl.multiple_of(j * chunk, chunk), chunk)
            part[b, :, cols] = dot32(hidden, down_full[:, cols]).astype(bf16)

        rc[b] = []
        for i, who in enumerate((lax.rem(c_peer + 2, tp_n), c_peer)):
            copy = send(part.at[b, pl.ds(who * half_mine, half_mine)], core_recv.at[b, i],
                        rc_ss.at[b, i], rc_rs.at[b, i], {"tp": c_peer})
            copy.start()
            rc[b].append(copy)

    def across(b):
        if b < 0:
            return
        for copy in rc[b]:
            copy.wait_recv()
        x_send[b] = (part[b, pl.ds(x_peer * half_mine, half_mine)].astype(f32)
                     + core_recv[b, 0].astype(f32)).astype(bf16)
        rx[b] = send(x_send.at[b], x_recv.at[b], rx_ss.at[b], rx_rs.at[b], {"tp": x_peer})
        rx[b].start()

    def home(b):
        if b < 0:
            return
        rx[b].wait_recv()
        term = (part[b, pl.ds(t * half_mine, half_mine)].astype(f32) + core_recv[b, 1].astype(f32)
                + x_recv[b].astype(f32))
        if b < 2:
            total[b * half_mine:(b + 1) * half_mine] = term
            return
        z_send[b] = term.astype(bf16)
        copy = send(z_send.at[b], z_recv.at[b], rz_ss.at[b], rz_rs.at[b], {"sp": behind(b // 2)})
        copy.start()
        rz.append(copy)

    spread(0)
    spread(1)
    forward_weights(sp_n - 1)
    cross(0)
    spread(2)
    own_up.wait()
    own_down.wait()
    for step in range(parts + 3):
        spread(step + 3)
        cross(step + 1)
        if step == 0:
            for copy in wy:
                copy.wait_recv()
        if step < parts:
            compute(step)
        if step - 1 < parts:
            across(step - 1)
        if step - 3 < parts:
            home(step - 3)
    for copy in rz:
        copy.wait_recv()
    for half in range(2):
        at = slice(half * half_mine, (half + 1) * half_mine)
        mixer = total[at]
        for d in range(1, sp_n):
            mixer = mixer + z_recv[2 * d + half].astype(f32)
        out[at] = (middle[at].astype(f32) + mixer).astype(bf16)
    for k in range(sp_n):
        for way in (1, -1):
            @pl.when(passes(k, way))
            def _():
                passing(k, way).wait_send()

    sent = [c for pair in wz for c in pair] + p_copy + wy + list(az.values()) + list(ax.values())
    sent += [c for pair in (*ac.values(), *rc.values()) for c in pair] + list(rx.values()) + rz
    for copy in sent:
        copy.wait_send()


def split_maps(query, masked):
    row_count, heads, both = query.shape
    half = both // 2
    if not masked:
        return query.reshape(row_count, heads * both)
    zero = jnp.zeros_like(query[:, :, :half])
    first = jnp.concatenate([query[:, :, :half], zero], axis=-1)
    second = jnp.concatenate([zero, query[:, :, half:]], axis=-1)
    return jnp.stack([first, second], axis=2).reshape(row_count, heads * 2 * both)


def fused(sizes, resid_in, query_narrow, key_narrow, value_narrow, query_wide, key_wide, value_wide,
          lambda_narrow, lambda_wide, head_gain, out_narrow, out_wide, norm_gain, up_weight, down_weight):
    grp_n, sp_n, tp_n = sizes
    bf16, f32 = jnp.bfloat16, jnp.float32
    q_parts, kv_parts, maps = [], [], []
    q_at = kv_at = 0
    for kind, (query, key, value) in enumerate(
            ((query_narrow, key_narrow, value_narrow), (query_wide, key_wide, value_wide))):
        rows, heads, both = query.shape
        kheads, v_width = key.shape[1], value.shape[2]
        half = both // 2
        masked = half % 128 != 0
        q_parts.append(split_maps(query, masked))
        kv_parts += [key.reshape(rows, kheads * both), value.reshape(rows, kheads * v_width)]
        for h in range(heads):
            kh = h // (heads // kheads)
            k0 = kv_at + kh * both
            v0 = kv_at + kheads * both + kh * v_width
            if masked:
                pair = tuple((q_at + (2 * h + c) * both, k0, both) for c in range(2))
            else:
                pair = tuple((q_at + h * both + c * half, k0 + c * half, half) for c in range(2))
            maps.append((pair, (kind, h), v0, half ** -0.5))
        q_at += q_parts[-1].shape[1]
        kv_at += kheads * (both + v_width)
    q = jnp.concatenate(q_parts, axis=1)
    kv = jnp.concatenate(kv_parts, axis=1)
    mine, width = resid_in.shape
    deep, hid = up_weight.shape[0], up_weight.shape[1] // sp_n
    vm, sm, anyw = (pl.BlockSpec(memory_space=m) for m in (pltpu.VMEM, pltpu.SMEM, pl.ANY))
    dma = pltpu.SemaphoreType.DMA
    n = sp_n
    scratch = [
        pltpu.VMEM((n * rows, kv.shape[1]), bf16),
        pltpu.VMEM((rows, len(maps) * v_width), bf16),
        pltpu.VMEM((rows, width), bf16),
        pltpu.VMEM((tp_n, mine, width), bf16),
        pltpu.VMEM((mine, width), bf16),
        pltpu.VMEM((n * rows, width), bf16),
        pltpu.VMEM((width, hid), bf16),
        pltpu.VMEM((hid, width), bf16),
        pltpu.VMEM((2 * n, rows // 2, width), bf16),
        pltpu.VMEM((2 * n, 2, mine // 2, width), bf16),
        pltpu.VMEM((2 * n, mine // 2, width), bf16),
        pltpu.VMEM((2 * n, mine // 2, width), bf16),
        pltpu.VMEM((2 * n, mine // 2, width), bf16),
        pltpu.VMEM((2 * n, mine // 2, width), bf16),
        pltpu.VMEM((mine, width), f32),
        dma((2, n)), dma((2, n)),
        dma((2, n)), dma((2, n)), dma((2, n)), dma((2, n)), dma((2,)),
        dma((tp_n,)), dma((tp_n,)),
        *(dma(k) for k in ((2 * n,), (2 * n,), (2, 2 * n)) for _ in range(2)),
        *(dma(k) for k in ((2 * n, 2), (2 * n,), (2 * n,)) for _ in range(2)),
    ]
    return pl.pallas_call(
        lambda *refs: layer_kernel((grp_n, sp_n, tp_n, tuple(maps)), *refs),
        out_shape=jax.ShapeDtypeStruct(resid_in.shape, bf16),
        in_specs=[vm, vm, vm, sm, sm, vm, vm, vm, vm, anyw, anyw],
        out_specs=vm,
        scratch_shapes=scratch,
        compiler_params=pltpu.CompilerParams(
            collective_id=0, has_side_effects=True, vmem_limit_bytes=VMEM_BYTES),
        name="layer",
    )(resid_in, q, kv, lambda_narrow, lambda_wide, head_gain[None], out_narrow, out_wide,
      norm_gain[None], up_weight, down_weight)


def fits(sizes, resid_in, query_narrow, up_weight):
    grp_n, sp_n, tp_n = sizes
    rows, width = query_narrow.shape[0], resid_in.shape[1]
    held = 2 * width * (3 * sp_n * rows + 2 * rows + 2 * up_weight.shape[1] // sp_n)
    return (grp_n == 2 and tp_n == 4 and up_weight.shape[1] % (sp_n * 256) == 0
            and up_weight.shape[0] % 256 == 0 and resid_in.shape[0] % 32 == 0 and held < VMEM_BYTES // 2)


def solution(mesh):
    placed = (
        P(("grp", "sp", "tp"), None),
        P(("grp", "sp"), "tp", None),
        P(("grp", "sp"), "tp", None),
        P(("grp", "sp"), "tp", None),
        P(("grp", "sp"), "tp", None),
        P(("grp", "sp"), "tp", None),
        P(("grp", "sp"), "tp", None),
        P("tp"),
        P("tp"),
        P(),
        P("tp", None),
        P("tp", None),
        P(),
        P("sp", "tp"),
        P("tp", "sp"),
    )
    sizes = tuple(mesh.shape[axis] for axis in ("grp", "sp", "tp"))

    def layer(*blocks):
        if fits(sizes, blocks[0], blocks[1], blocks[13]):
            return fused(sizes, *blocks)
        return shards(*blocks)

    return jax.shard_map(
        layer, mesh=mesh, in_specs=placed, out_specs=P(("grp", "sp", "tp"), None), check_vma=False
    )
```
